512 devices in a mesh: kv: 16 (over y, x), tp: 32 (over z, core).
Axes of the slice: x: 4, y: 4, z: 16, core: 2. Of those that a mesh axis runs over, the one named last changes fastest.
Arguments:
- tokens: bfloat16 [64, 4096], P(None, ('kv', 'tp')), may hold values from -9 to 9
- lengths: int32 [64], replicated, may hold values from 1 to 16384, 262144 in all
- gain_attn: float32 [4096], P('kv'), may hold values from 0.1 to 1.9
- w_query_nope: bfloat16 [4096, 4096], P('kv', 'tp'), may hold values from -0.09375 to 0.09375
- w_query_rope: bfloat16 [4096, 2048], P('kv', 'tp'), may hold values from -0.09375 to 0.09375
- w_latent: bfloat16 [4096, 512], P('kv'), may hold values from -0.09375 to 0.09375
- w_rope_key: bfloat16 [4096, 64], P('kv'), may hold values from -0.09375 to 0.09375
- gain_latent: float32 [512], replicated, may hold values from 0.1 to 1.9
- w_key_up: bfloat16 [512, 4096], P(None, 'tp'), may hold values from -0.75 to 0.75
- w_value_up: bfloat16 [512, 4096], P(None, 'tp'), may hold values from -0.25 to 0.25
- w_out: bfloat16 [4096, 4096], P('tp', 'kv'), may hold values from -0.25 to 0.25
- gain_mlp: float32 [4096], P('kv'), may hold values from 0.1 to 1.9
- w_up: bfloat16 [4096, 16384], P('kv', 'tp'), may hold values from -0.09375 to 0.09375
- w_down: bfloat16 [16384, 4096], P('tp', 'kv'), may hold values from -0.046875 to 0.046875
- cache_latent: bfloat16 [64, 16384, 512], P('tp', 'kv'), may hold values from -6 to 6
- cache_rope: bfloat16 [64, 16384, 64], P('tp', 'kv'), may hold values from -900 to 900
Outputs:
- mixed: bfloat16 [64, 4096], P(None, ('kv', 'tp'))
The draws below stay inside these ranges and needn't reach their ends.
Inputs may be any that keep to these rules, and one draw needn't show every extreme that they name: `lengths`: one sequence has exactly 16384 live positions.
All inputs are finite; a program needn't handle non-finite values.
Results may differ from the reference program's by a relative error of at most 0.035.
The reference program's roundings to bfloat16 on the way count: a program that leaves them out, or rounds other values in their place, can miss the bound.
Values may be sent and summed in bfloat16 or wider, within the bound.
No kernel may reach another device: no remote copies, remote signals or barrier semaphores. Data moves between devices by JAX's collectives and lax.ppermute only.
A program may use at most 64 MiB of HBM per device.

```python
import math
import jax
import jax.numpy as jnp
import numpy as np
from jax import lax

D = 4096
H = 32
NOPE = 128
ROPE = 64
VD = 128
RANK = 512
FF = 16384
CACHE_DEV = 1024
BATCH = 64
CACHE = 16384
N_KV = 16


def draw_tokens(key, part):
    column_scale = 0.5 * 3.0 ** (jnp.arange(D, dtype=jnp.float32) / D)
    values = jnp.clip(jax.random.normal(key, (BATCH, D), jnp.float32), -6.0, 6.0)
    return (values * column_scale).astype(jnp.bfloat16)


def draw_cache_rope(key, part):
    values = jnp.clip(jax.random.normal(key, (BATCH, CACHE, ROPE), jnp.float32), -6.0, 6.0)
    return values.astype(jnp.bfloat16)


def block_levels(key, shape, split, low, top_value):
    def one(position, shards_of):
        heights = jax.random.uniform(jax.random.fold_in(jax.random.fold_in(key, 6), position), (shards_of,), jnp.float32, low / len(split), top_value / len(split))
        return jnp.repeat(jnp.exp(heights), shape[position] // shards_of).reshape((-1,) + (1,) * (len(shape) - position - 1))

    level = one(*split[0])
    for cut in split[1:]:
        level = level * one(*cut)
    return level


def profile(count, total, limit, lean):
    portions = [(1 << 20) // math.isqrt(grade ** lean) + 1 for grade in range(2, count + 1)]
    surplus, counts = total - limit - (count - 1), [1] * (count - 1)
    while surplus > 0:
        candidates = [i for i in range(count - 1) if counts[i] < limit]
        mass, left = sum([portions[i] for i in candidates]), surplus
        for i in candidates:
            addition = min(limit - counts[i], max(1, left * portions[i] // mass), surplus)
            counts[i] = counts[i] + addition
            surplus = surplus - addition
    return np.array([limit] + counts)


def uneven_parts(rng, count, total, limit, skew):
    if count == 2:
        one = jax.random.randint(rng, (), max(1, total - limit), min(limit, total - 1) + 1)
        return jnp.stack([one, total - one])
    sizes = jnp.asarray(profile(count, total, limit, skew), jnp.int32)
    pairs = (count - 1) // 2
    source_of, sink = sizes[1:1 + 2 * pairs:2], sizes[2:2 + 2 * pairs:2]
    room = jnp.minimum(source_of - 1, limit - sink)
    moved = jax.random.randint(jax.random.fold_in(rng, 1), (pairs,), 0, 1 << 20) % (room + 1)
    sizes = sizes.at[1:1 + 2 * pairs:2].set(source_of - moved).at[2:2 + 2 * pairs:2].set(sink + moved)
    return sizes[jax.random.permutation(jax.random.fold_in(rng, 2), count)]


def centred(stream_key, dims, deviation, limit, shards=(), kind=jnp.bfloat16):
    values = jax.random.normal(stream_key, dims, jnp.float32) * deviation
    if len(shards) > 0:
        values = block_levels(stream_key, dims, shards, -0.22, 0.18) * values
    return jnp.clip(values, min=-limit, max=limit).astype(kind)


def setup_inputs(seed: int = 0) -> dict:
    arg_keys = jax.random.split(jax.random.key(seed), 17)
    tokens = draw_tokens(jax.random.fold_in(arg_keys[16], 71), 0)
    lengths = uneven_parts(arg_keys[1], BATCH, BATCH * CACHE // 4, CACHE, 2).astype(jnp.int32)
    gain_attn = jnp.clip(1.0 + 0.18 * jax.random.normal(arg_keys[2], (D,), jnp.float32), 0.1, 1.9)
    w_query_nope = centred(arg_keys[3], (D, H * NOPE), D ** -0.5, 0.09375, ((0, 16), (1, 32)))
    w_query_rope = centred(arg_keys[4], (D, H * ROPE), D ** -0.5, 0.09375, ((0, 16), (1, 32)))
    w_latent = centred(arg_keys[5], (D, RANK), D ** -0.5, 0.09375, ((0, 16),))
    w_rope_key = centred(arg_keys[6], (D, ROPE), D ** -0.5, 0.09375, ((0, 16),))
    gain_latent = jnp.clip(1.0 + 0.18 * jax.random.normal(arg_keys[7], (RANK,), jnp.float32), 0.1, 1.9)
    w_key_up = centred(arg_keys[8], (RANK, H * NOPE), (RANK // 8) ** -0.5, 0.75, ((1, 32),))
    w_value_up = centred(arg_keys[9], (RANK, H * VD), RANK ** -0.5, 0.25, ((1, 32),))
    w_out = centred(arg_keys[10], (H * VD, D), (H * VD // 8) ** -0.5, 0.25, ((0, 32), (1, 16)))
    gain_mlp = jnp.clip(1.0 + 0.18 * jax.random.normal(arg_keys[11], (D,), jnp.float32), 0.1, 1.9)
    w_up = centred(arg_keys[12], (D, FF), D ** -0.5, 0.09375, ((0, 16), (1, 32)))
    w_down = centred(arg_keys[13], (FF, D), FF ** -0.5, 0.046875, ((0, 32), (1, 16)))
    cache_latent = centred(arg_keys[14], (BATCH, CACHE, RANK), 1.0, 6.0, ((0, 32), (1, 16)))
    cache_rope = draw_cache_rope(jax.random.fold_in(arg_keys[16], 71), 0)
    return {"tokens": tokens, "lengths": lengths, "gain_attn": gain_attn, "w_query_nope": w_query_nope, "w_query_rope": w_query_rope, "w_latent": w_latent, "w_rope_key": w_rope_key, "gain_latent": gain_latent, "w_key_up": w_key_up, "w_value_up": w_value_up, "w_out": w_out, "gain_mlp": gain_mlp, "w_up": w_up, "w_down": w_down, "cache_latent": cache_latent, "cache_rope": cache_rope}


EPS = 1e-06

def rotate(values, positions):
    half_dim = values.shape[-1] // 2
    inv_freq = 10000.0 ** (-jnp.arange(half_dim, dtype=jnp.float32) / half_dim)
    angles = positions.astype(jnp.float32)[..., None] * inv_freq
    cos_part = jnp.cos(angles)
    sin_part = jnp.sin(angles)
    lower = values[..., :half_dim]
    upper = values[..., half_dim:]
    return jnp.concatenate([lower * cos_part - upper * sin_part, upper * cos_part + lower * sin_part], axis=-1)

def reference(tokens, lengths, gain_attn, w_query_nope, w_query_rope, w_latent, w_rope_key, gain_latent, w_key_up, w_value_up, w_out, gain_mlp, w_up, w_down, cache_latent, cache_rope):
    batch_rows = tokens.shape[0]
    widened = tokens.astype(jnp.float32)
    inv_rms = lax.rsqrt(lax.optimization_barrier(jnp.mean(widened * widened, axis=1)) + EPS)
    scaled = (widened * gain_attn.astype(jnp.float32)).astype(jnp.bfloat16)
    q_nope = (jnp.dot(scaled, w_query_nope, preferred_element_type=jnp.float32) * inv_rms[:, None]).astype(jnp.bfloat16).reshape(batch_rows, H, NOPE)
    rope_raw = (jnp.dot(scaled, w_query_rope, preferred_element_type=jnp.float32) * inv_rms[:, None]).reshape(batch_rows, H, ROPE)
    q_rope = rotate(rope_raw, lengths[:, None]).astype(jnp.bfloat16)
    raw_latent = jnp.dot(scaled, w_latent, preferred_element_type=jnp.float32) * inv_rms[:, None]
    latent_new = (raw_latent * lax.rsqrt(lax.optimization_barrier(jnp.mean(raw_latent * raw_latent, axis=1, keepdims=True)) + EPS) * gain_latent.astype(jnp.float32)).astype(jnp.bfloat16)
    key_new = rotate(jnp.dot(scaled, w_rope_key, preferred_element_type=jnp.float32) * inv_rms[:, None], lengths).astype(jnp.bfloat16)
    key_up = w_key_up.reshape(RANK, H, NOPE).astype(jnp.float32)
    q_latent = jnp.einsum('bhn,rhn->bhr', q_nope.astype(jnp.float32), key_up).astype(jnp.bfloat16)
    score_scale = (NOPE + ROPE) ** (-0.5)

    def attend(sequence_data):
        latent_query, rope_query, latent_rows, rope_rows, live_len, own_latent, own_key = sequence_data
        positions = jnp.arange(CACHE, dtype=jnp.int32)
        rotated = rotate(rope_rows.astype(jnp.float32), positions).astype(jnp.bfloat16)
        scores = (jnp.dot(latent_query, latent_rows.T, preferred_element_type=jnp.float32) + jnp.dot(rope_query, rotated.T, preferred_element_type=jnp.float32)) * score_scale
        live_mask = (positions < live_len).reshape(N_KV, CACHE_DEV)
        blocks = scores.reshape(H, N_KV, CACHE_DEV)
        block_max = lax.optimization_barrier(jnp.max(jnp.where(live_mask[None], blocks, -1e+30), axis=2))
        exponent = jnp.where(live_mask[None], jnp.exp(blocks - block_max[..., None]), 0.0)
        block_sum = lax.optimization_barrier(jnp.sum(exponent, axis=2))
        expo_low = lax.optimization_barrier(exponent.astype(jnp.bfloat16))
        weighted = jnp.einsum('hjp,jpr->hjr', expo_low.astype(jnp.float32), latent_rows.reshape(N_KV, CACHE_DEV, RANK).astype(jnp.float32))
        block_out = lax.optimization_barrier((weighted / jnp.where(block_sum > 0, block_sum, 1.0)[..., None]).astype(jnp.bfloat16))
        own_score = (jnp.dot(latent_query, own_latent, preferred_element_type=jnp.float32) + jnp.dot(rope_query, own_key, preferred_element_type=jnp.float32)) * score_scale
        new_max = jnp.maximum(lax.optimization_barrier(jnp.max(block_max, axis=1)), own_score)
        block_weight = block_sum * jnp.exp(block_max - new_max[:, None])
        own_weight = jnp.exp(own_score - new_max)
        result = (lax.optimization_barrier(jnp.sum(block_weight[..., None] * block_out.astype(jnp.float32), axis=1)) + own_weight[:, None] * own_latent.astype(jnp.float32)[None, :]) / (lax.optimization_barrier(jnp.sum(block_weight, axis=1)) + own_weight)[:, None]
        return result.astype(jnp.bfloat16)
    o_latent = lax.map(attend, (q_latent, q_rope, cache_latent, cache_rope, lengths, latent_new, key_new))
    value_up = w_value_up.reshape(RANK, H, VD).astype(jnp.float32)
    head_out = jnp.einsum('bhr,rhv->bhv', o_latent.astype(jnp.float32), value_up).astype(jnp.bfloat16).reshape(batch_rows, H * VD)
    resid = (widened + jnp.dot(head_out, w_out, preferred_element_type=jnp.float32)).astype(jnp.bfloat16)
    resid_wide = resid.astype(jnp.float32)
    inv_rms2 = lax.rsqrt(lax.optimization_barrier(jnp.mean(resid_wide * resid_wide, axis=1)) + EPS)
    scaled2 = (resid_wide * gain_mlp.astype(jnp.float32)).astype(jnp.bfloat16)
    up_sum = jnp.dot(scaled2, w_up, preferred_element_type=jnp.float32)
    activated = jnp.square(jnp.maximum(up_sum, 0.0)).astype(jnp.bfloat16)
    down_sum = jnp.dot(activated, w_down, preferred_element_type=jnp.float32)
    return (resid_wide + (inv_rms2 * inv_rms2)[:, None] * down_sum).astype(jnp.bfloat16)
```

```python
import jax
import jax.numpy as jnp
from jax import lax
from jax.sharding import Mesh
from jax.sharding import PartitionSpec as P

D = 4096
NOPE = 128
ROPE = 64
VD = 128
RANK = 512
KV = ("kv_0", "kv_1")
KV_TP = ("kv_0", "kv_1", "tp")
EPS = 1e-06
BF = jnp.bfloat16
F32 = jnp.float32


def exchange(parts, axis):
    return lax.all_to_all(parts, axis, 0, 0, tiled=True)


def to_all(value, axis):
    peers = lax.axis_size(axis)
    return exchange(jnp.broadcast_to(value[None], (peers, *value.shape)), axis)


def split3(x):
    hi = lax.reduce_precision(x, 8, 7)
    rest = x - hi
    mid = lax.reduce_precision(rest, 8, 7)
    low = rest - mid
    return hi.astype(BF), mid.astype(BF), low.astype(BF)


def join3(hi, mid, low):
    return hi.astype(F32) + (mid.astype(F32) + low.astype(F32))


def rotate(values, positions):
    half_dim = values.shape[-1] // 2
    inv_freq = 10000.0 ** (-jnp.arange(half_dim, dtype=F32) / half_dim)
    angles = positions.astype(F32)[..., None] * inv_freq
    cos_part = jnp.cos(angles)
    sin_part = jnp.sin(angles)
    lower = values[..., :half_dim]
    upper = values[..., half_dim:]
    return jnp.concatenate(
        [lower * cos_part - upper * sin_part, upper * cos_part + lower * sin_part], axis=-1
    )


def per_device(
    tokens,
    lengths,
    gain_attn,
    w_query_nope,
    w_query_rope,
    w_latent,
    w_rope_key,
    gain_latent,
    w_key_up,
    w_value_up,
    w_out,
    gain_mlp,
    w_up,
    w_down,
    cache_latent,
    cache_rope,
):
    kv_index = lax.axis_index(KV)
    tp_index = lax.axis_index("tp")
    n_kv = lax.axis_size(KV)
    n_tp = lax.axis_size("tp")
    seq_dev, cache_dev = cache_latent.shape[:2]
    batch = tokens.shape[0]

    block_t = to_all(tokens.T, "tp").reshape(-1, batch)
    wide_t = block_t.astype(F32)
    square_piece = jnp.sum(wide_t * wide_t, axis=0)
    scaled_t = (wide_t * gain_attn[:, None]).astype(BF)
    dims = (((0,), (0,)), ((), ()))
    part_nope = lax.dot_general(scaled_t, w_query_nope, dims, preferred_element_type=F32)
    part_rope = lax.dot_general(scaled_t, w_query_rope, dims, preferred_element_type=F32)
    own_rows = lax.dynamic_slice_in_dim(scaled_t, tp_index * seq_dev, seq_dev, 1)
    part_latent = lax.dot_general(own_rows, w_latent, dims, preferred_element_type=F32)
    part_key = lax.dot_general(own_rows, w_rope_key, dims, preferred_element_type=F32)
    lane = 128
    pieces = [part_nope, part_rope, part_latent, part_key, square_piece]
    flat = [
        jnp.pad(p.reshape(-1), (0, -p.size % lane)).reshape(-1, lane).astype(BF) for p in pieces
    ]
    rows = [f.shape[0] for f in flat]
    packed = jnp.concatenate(flat, axis=0)
    packed = jnp.pad(packed, ((0, -packed.shape[0] % 16), (0, 0)))
    total = jnp.sum(to_all(packed, KV).astype(F32), axis=0)
    at = 0
    sums = []
    for p, r in zip(pieces, rows):
        sums.append(total[at : at + r].reshape(-1)[: p.size].reshape(p.shape))
        at += r
    nope_sum, rope_sum, latent_sum, key_sum, square_sum = sums
    inv_rms = lax.rsqrt(square_sum / D + EPS)
    q_nope = (nope_sum * inv_rms[:, None]).astype(BF)
    q_rope = rotate(rope_sum * inv_rms[:, None], lengths).astype(BF)
    q_latent = lax.dot_general(
        q_nope, w_key_up, (((1,), (1,)), ((), ())), preferred_element_type=F32
    ).astype(BF)
    query = jnp.concatenate([q_latent, q_rope], axis=1)
    query = exchange(query.reshape(n_tp, seq_dev, RANK + ROPE), "tp")
    latent_query = jnp.swapaxes(query[:, :, :RANK], 0, 1)
    rope_query = jnp.swapaxes(query[:, :, RANK:], 0, 1)

    own_inv = lax.dynamic_slice_in_dim(inv_rms, tp_index * seq_dev, seq_dev, 0)
    own_len = lax.dynamic_slice_in_dim(lengths, tp_index * seq_dev, seq_dev, 0)
    raw_latent = latent_sum * own_inv[:, None]
    latent_new = (
        raw_latent
        * lax.rsqrt(jnp.mean(raw_latent * raw_latent, axis=1, keepdims=True) + EPS)
        * gain_latent
    ).astype(BF)
    key_new = rotate(key_sum * own_inv[:, None], own_len).astype(BF)

    score_scale = (NOPE + ROPE) ** (-0.5)
    positions = kv_index * cache_dev + jnp.arange(cache_dev, dtype=jnp.int32)
    rotated = rotate(cache_rope.astype(F32), positions).astype(BF)
    scores = (
        jnp.einsum("shr,spr->shp", latent_query, cache_latent, preferred_element_type=F32)
        + jnp.einsum("shk,spk->shp", rope_query, rotated, preferred_element_type=F32)
    ) * score_scale
    own_score = (
        jnp.einsum("shr,sr->sh", latent_query, latent_new, preferred_element_type=F32)
        + jnp.einsum("shk,sk->sh", rope_query, key_new, preferred_element_type=F32)
    ) * score_scale
    first = kv_index == 0
    own_score = jnp.where(first, own_score, -1e30)
    live = positions[None, None, :] < own_len[:, None, None]
    peak = jnp.maximum(jnp.max(jnp.where(live, scores, -1e30), axis=2), own_score)
    expo = jnp.where(live, jnp.exp(scores - peak[..., None]), 0.0)
    own_weight = jnp.where(first, jnp.exp(own_score - peak), 0.0)
    mass = jnp.sum(expo, axis=2) + own_weight
    weighted = jnp.einsum(
        "shp,spr->shr", expo.astype(BF), cache_latent, preferred_element_type=F32
    )
    weighted = weighted + own_weight[..., None] * latent_new.astype(F32)[:, None, :]
    block_out = (weighted / jnp.where(mass > 0, mass, 1.0)[..., None]).astype(BF)

    stats = jnp.stack([*split3(peak), *split3(mass)], axis=-1)
    stats = jnp.pad(stats, ((0, 0), (0, 0), (0, lane - stats.shape[-1])))
    sent = jnp.concatenate([block_out, stats], axis=-1)
    got = exchange(jnp.swapaxes(sent, 0, 1), "tp").reshape(batch, RANK + lane)
    head_part = jnp.dot(got[:, :RANK], w_value_up, preferred_element_type=F32).astype(BF)
    both = jnp.concatenate([head_part, got[:, RANK:]], axis=1)
    blocks = to_all(both, KV)
    peaks = join3(blocks[:, :, VD], blocks[:, :, VD + 1], blocks[:, :, VD + 2])
    masses = join3(blocks[:, :, VD + 3], blocks[:, :, VD + 4], blocks[:, :, VD + 5])
    top = jnp.max(peaks, axis=0)
    weight = masses * jnp.exp(peaks - top)
    weight = weight / jnp.sum(weight, axis=0)
    head_out = jnp.sum(weight[..., None] * blocks[:, :, :VD].astype(F32), axis=0).astype(BF)

    attn_part = jnp.dot(head_out, w_out, preferred_element_type=F32).astype(BF)
    width = attn_part.shape[1]
    attn_rows = jnp.sum(
        exchange(attn_part.reshape(n_tp, seq_dev, width), "tp").astype(F32), axis=0
    )
    own_cols = lax.dynamic_slice_in_dim(block_t, tp_index * seq_dev, seq_dev, 1)
    resid_rows = (own_cols.T.astype(F32) + attn_rows).astype(BF)
    resid = to_all(resid_rows, "tp").reshape(batch, width)
    resid_wide = resid.astype(F32)
    square_two = jnp.sum(resid_wide * resid_wide, axis=1, keepdims=True)
    scaled2 = (resid_wide * gain_mlp).astype(BF)
    up_part = jnp.dot(scaled2, w_up, preferred_element_type=F32)
    units = up_part.shape[1]
    up_sent = jnp.concatenate(
        [up_part, jnp.broadcast_to(square_two, (batch, lane))], axis=1
    ).astype(BF)
    up_got = exchange(up_sent.reshape(n_kv, batch // n_kv, units + lane), KV)
    up_all = jnp.sum(up_got.astype(F32), axis=0)
    inv_rms2 = lax.rsqrt(up_all[:, units:units + 1] / D + EPS)
    active = jnp.square(jnp.maximum(up_all[:, :units], 0.0) * inv_rms2).astype(BF)
    activated = to_all(active, KV).reshape(batch, units)
    down_t = lax.dot_general(
        w_down, activated, (((0,), (1,)), ((), ())), preferred_element_type=F32
    ).astype(BF)
    out_cols = width // n_tp
    down_sum = jnp.sum(
        exchange(down_t.reshape(n_tp, out_cols, batch), "tp").astype(F32), axis=0
    )
    resid_cols = lax.dynamic_slice_in_dim(resid_wide, tp_index * out_cols, out_cols, 1)
    return (resid_cols + down_sum.T).astype(BF)


def solution(mesh):
    split = Mesh(mesh.devices.reshape(4, 4, mesh.shape["tp"]), ("kv_0", "kv_1", "tp"))
    in_specs = (
        P(None, KV_TP),
        P(),
        P(KV),
        P(KV, "tp"),
        P(KV, "tp"),
        P(KV, None),
        P(KV, None),
        P(),
        P(None, "tp"),
        P(None, "tp"),
        P("tp", KV),
        P(KV),
        P(KV, "tp"),
        P("tp", KV),
        P("tp", KV, None),
        P("tp", KV, None),
    )
    out_specs = P(None, KV_TP)
    return jax.shard_map(
        per_device, mesh=split, in_specs=in_specs, out_specs=out_specs, check_vma=False
    )
```

```python
import jax
import jax.numpy as jnp
from jax import lax
from jax.experimental import pallas as pl
from jax.experimental.pallas import tpu as pltpu
from jax.sharding import Mesh
from jax.sharding import PartitionSpec as P

D = 4096
NOPE = 128
ROPE = 64
VD = 128
RANK = 512
LANE = 128
KV = ("kv_0", "kv_1")
KV_TP = ("kv_0", "kv_1", "tp")
EPS = 1e-06
BF = jnp.bfloat16
F32 = jnp.float32
NT = (((1,), (1,)), ((), ()))


def exchange(parts, axis):
    return lax.all_to_all(parts, axis, 0, 0, tiled=True)


def mm(a, b):
    return jnp.dot(a, b, preferred_element_type=F32)


def mm_nt(a, b):
    return lax.dot_general(a, b, NT, preferred_element_type=F32)


def split3(x):
    hi = x.astype(BF).astype(F32)
    rest = x - hi
    mid = rest.astype(BF).astype(F32)
    return hi, mid, rest - mid


def as_column(row):
    n = row.shape[1]
    full = jnp.broadcast_to(row, (LANE, n))
    return jnp.transpose(full)


def one_hot_rows(first, rows, columns):
    row = lax.broadcasted_iota(jnp.int32, (rows, columns), 0)
    column = lax.broadcasted_iota(jnp.int32, (rows, columns), 1)
    return jnp.where(column == first + row, 1.0, 0.0).astype(BF)


def read_pairs(ref, scratch):
    n, two, _ = ref.shape
    for i in range(n):
        scratch[two * i : two * (i + 1), :] = ref[i].astype(F32)
    return scratch[...]


def write_pairs(ref, scratch, value):
    n, two, _ = ref.shape
    scratch[...] = value
    for i in range(n):
        ref[i] = scratch[two * i : two * (i + 1), :].astype(BF)


def stage_query(at, got, gain, w_nope, w_rope, w_latent, w_key, out, own_out):
    n_tp, four, _ = got.shape
    seq_dev = own_out.shape[0]
    x = got[...].astype(F32)
    batch = LANE // 2
    block_t = jnp.concatenate([x[:, :, :batch], x[:, :, batch:]], axis=1)
    block_t = block_t.reshape(n_tp * 2 * four, batch)
    squares = jnp.sum(block_t * block_t, axis=0, keepdims=True)
    block = jnp.transpose(block_t)
    scaled = (block * gain[...]).astype(BF)
    nope = mm(scaled, w_nope[...])
    rope = mm(scaled, w_rope[...])
    pick = one_hot_rows(at[1] * seq_dev, 8, batch)
    own = mm(pick, scaled).astype(BF)
    own_out[...] = mm(pick, block.astype(BF))[:seq_dev]
    latent = mm(own, w_latent[...])
    key = mm(own, w_key[...])
    half = batch // 2
    rows = [
        nope,
        jnp.concatenate([rope[:half], rope[half:]], axis=1),
        *[latent[:2, LANE * j : LANE * (j + 1)] for j in range(RANK // LANE)],
        jnp.concatenate([key[0:1], key[1:2]], axis=1),
        jnp.concatenate([squares, squares], axis=1),
        jnp.zeros((6, LANE), F32),
    ]
    packed = jnp.concatenate(rows, axis=0).astype(BF)
    for j in range(out.shape[0]):
        out[j] = packed


def turned(values, cos_ref, sin_ref):
    half = values.shape[1] // 2
    swapped = jnp.concatenate([values[:, half:], values[:, :half]], axis=1)
    return values * cos_ref + swapped * sin_ref


def stage_absorb(at, got, w_key_up, gain_latent, cos_len, sin_len, out, new_out, scratch, trig):
    total = got[0].astype(F32)
    for j in range(1, got.shape[0]):
        total = total + got[j].astype(F32)
    batch = w_key_up.shape[1] // 2
    half = batch // 2
    nope = total[:batch]
    packed = total[batch : batch + half]
    rope = jnp.concatenate([packed[:, :ROPE], packed[:, ROPE:]], axis=0)
    at_row = batch + half
    latent = jnp.concatenate([total[at_row + 2 * j : at_row + 2 * j + 2] for j in range(4)], axis=1)
    key = total[at_row + 8 : at_row + 9]
    key = jnp.concatenate([key[:, :ROPE], key[:, ROPE:]], axis=0)
    squares = total[at_row + 9 : at_row + 10, :batch]
    inv = as_column(lax.rsqrt(squares / D + EPS))
    q_nope = (nope * inv).astype(BF)
    q_rope = turned(rope * inv[:, :ROPE], cos_len[...], sin_len[...])
    q_latent = mm_nt(q_nope, w_key_up[...])
    value = jnp.concatenate([q_latent, q_rope, jnp.zeros_like(q_rope)], axis=1)
    write_pairs(out, scratch, value)
    first = at[1] * 2
    trig[0] = inv
    trig[1] = jnp.concatenate([cos_len[...], sin_len[...]], axis=1)
    own_inv = trig[0, pl.ds(first, 2), :]
    own_trig = trig[1, pl.ds(first, 2), :]
    raw = latent * own_inv[:, :1]
    norm = lax.rsqrt(jnp.mean(raw * raw, axis=1, keepdims=True) + EPS)
    latent_new = raw * norm * gain_latent[...]
    key_new = turned(key * own_inv[:, :ROPE], own_trig[:, :ROPE], own_trig[:, ROPE:])
    new_out[...] = (
        jnp.concatenate([latent_new, key_new, jnp.zeros_like(key_new)], axis=1)
        .astype(BF)
        .astype(F32)
    )


def stage_attend(at, got, cache, rotated, new, out, scratch):
    query = read_pairs(got, scratch)
    rows = query.shape[0]
    cache_dev = cache.shape[1]
    latent_query = query[:, :RANK].astype(BF)
    rope_query = query[:, RANK : RANK + ROPE].astype(BF)
    even_column = lax.broadcasted_iota(jnp.int32, (rows, 1), 0) % 2 == 0
    scale = (NOPE + ROPE) ** (-0.5)
    each = [
        mm_nt(latent_query, cache[s]) + mm_nt(rope_query, rotated[s]) for s in range(2)
    ]
    scores = jnp.where(even_column, each[0], each[1]) * scale
    length = jnp.where(even_column, at[2], at[3])
    position = at[0] * cache_dev + lax.broadcasted_iota(jnp.int32, scores.shape, 1)
    live = position < length
    new_rows = jnp.where(even_column, new[0:1], new[1:2])
    own = jnp.sum(query * new_rows, axis=1, keepdims=True) * scale
    first = at[0] == 0
    peak = jnp.max(jnp.where(live, scores, -1e30), axis=1, keepdims=True)
    peak = jnp.where(first, jnp.maximum(peak, own), peak)
    expo = jnp.where(live, jnp.exp(scores - peak), 0.0)
    own_weight = jnp.where(first, jnp.exp(own - peak), 0.0)
    mass = jnp.sum(expo, axis=1, keepdims=True) + own_weight
    low = [
        jnp.where(even_column, expo, 0.0).astype(BF),
        jnp.where(even_column, 0.0, expo).astype(BF),
    ]
    weighted = mm(low[0], cache[0]) + mm(low[1], cache[1])
    weighted = weighted + own_weight * new_rows[:, :RANK]
    block_out = weighted / jnp.where(mass > 0, mass, 1.0)
    lane = lax.broadcasted_iota(jnp.int32, (rows, LANE), 1)
    stats = jnp.zeros((rows, LANE), F32)
    for i, piece in enumerate((*split3(peak), *split3(mass))):
        stats = jnp.where(lane == i, piece, stats)
    write_pairs(out, scratch, jnp.concatenate([block_out, stats], axis=1))


def stage_heads(got, w_value_up, out, scratch):
    value = read_pairs(got, scratch)
    part = mm(value[:, :RANK].astype(BF), w_value_up[...])
    stats = jnp.transpose(value[:, RANK:])[:16]
    stats = jnp.concatenate([stats, jnp.zeros_like(stats)], axis=1)
    packed = jnp.concatenate([part, stats], axis=0).astype(BF)
    for j in range(out.shape[0]):
        out[j] = packed


def stage_project(got, w_out, out, scratch):
    blocks, rows, _ = got.shape
    batch = rows - 16
    stats = got[:, batch:, :].astype(F32)
    peak = stats[:, 0] + (stats[:, 1] + stats[:, 2])
    mass = stats[:, 3] + (stats[:, 4] + stats[:, 5])
    top = jnp.max(peak, axis=0, keepdims=True)
    weight = mass * jnp.exp(peak - top)
    total = jnp.sum(weight, axis=0, keepdims=True)
    weight = weight / jnp.where(total > 0, total, 1.0)
    weight = jnp.concatenate([weight, jnp.zeros((LANE - blocks, LANE), F32)], axis=0)
    column = jnp.transpose(weight)[:batch]
    head = column[:, 0:1] * got[0, :batch].astype(F32)
    for j in range(1, blocks):
        head = head + column[:, j : j + 1] * got[j, :batch].astype(F32)
    write_pairs(out, scratch, mm(head.astype(BF), w_out[...]))


def stage_resid(got, own, out):
    total = own[...]
    for i in range(got.shape[0]):
        total = total + got[i].astype(F32)
    total = total.astype(BF)
    for i in range(out.shape[0]):
        out[i] = total


def stage_up(at, got, gain, w_up, out, own_out, scratch):
    resid = read_pairs(got, scratch)
    batch, width = resid.shape
    squares = jnp.sum(resid * resid, axis=1, keepdims=True)
    square_rows = jnp.transpose(jnp.broadcast_to(squares, (batch, LANE)))[:8]
    scaled = (resid * gain[...]).astype(BF)
    up = mm(scaled, w_up[...])
    units = up.shape[1]
    extra = jnp.concatenate([square_rows, jnp.zeros((8, units - batch), F32)], axis=1)
    packed = jnp.concatenate([up, extra], axis=0).astype(BF)
    for j in range(out.shape[0]):
        out[j] = packed
    pick = one_hot_rows(at[1] * 8, 8, width)
    own_out[...] = mm_nt(pick, resid.astype(BF))


def stage_down(got, w_down, out):
    total = got[0].astype(F32)
    for j in range(1, got.shape[0]):
        total = total + got[j].astype(F32)
    batch = total.shape[0] - 8
    active = jnp.square(jnp.maximum(total[:batch], 0.0)).astype(BF)
    inv = lax.rsqrt(total[batch : batch + 1, :batch] / D + EPS)
    down = jnp.transpose(mm(active, w_down[...])) * (inv * inv)
    n_tp = out.shape[0]
    down = down.reshape(n_tp, -1, batch)
    half = down.shape[1] // 2
    out[...] = jnp.concatenate([down[:, :half], down[:, half:]], axis=2).astype(BF)


def stage_last(got, own, out):
    total = jnp.sum(got[...].astype(F32), axis=0)
    batch = own.shape[1]
    value = jnp.concatenate([total[:, :batch], total[:, batch:]], axis=0) + own[...]
    value = jnp.concatenate([value, jnp.zeros_like(value)], axis=1)
    out[...] = jnp.transpose(value)[:batch].astype(BF)


def call(body, outs, operands, scratch=(), scalars=True):
    specs = [pl.BlockSpec(memory_space=pltpu.VMEM) for _ in operands]
    if scalars:
        specs[0] = pl.BlockSpec(memory_space=pltpu.SMEM)
    made = pl.pallas_call(
        body,
        out_shape=[jax.ShapeDtypeStruct(s, t) for s, t in outs],
        in_specs=specs,
        out_specs=[pl.BlockSpec(memory_space=pltpu.VMEM) for _ in outs],
        scratch_shapes=[pltpu.VMEM(s, F32) for s in scratch],
        name=body.__name__,
    )(*operands)
    return made if len(outs) > 1 else made[0]


def angles_of(positions):
    half_dim = ROPE // 2
    inv_freq = 10000.0 ** (-jnp.arange(half_dim, dtype=F32) / half_dim)
    angles = positions.astype(F32)[..., None] * inv_freq
    return jnp.cos(angles), jnp.sin(angles)


def per_device(
    tokens,
    lengths,
    gain_attn,
    w_query_nope,
    w_query_rope,
    w_latent,
    w_rope_key,
    gain_latent,
    w_key_up,
    w_value_up,
    w_out,
    gain_mlp,
    w_up,
    w_down,
    cache_latent,
    cache_rope,
):
    kv_index = lax.axis_index(KV)
    tp_index = lax.axis_index("tp")
    n_kv = lax.axis_size(KV)
    n_tp = lax.axis_size("tp")
    seq_dev, cache_dev = cache_latent.shape[:2]
    batch, out_cols = tokens.shape
    width = w_out.shape[1]
    units = w_up.shape[1]
    own_len = lax.dynamic_slice_in_dim(lengths, tp_index * seq_dev, seq_dev, 0)
    at = jnp.concatenate(
        [jnp.stack([kv_index, tp_index]).astype(jnp.int32), own_len.astype(jnp.int32)]
    )

    turned_tokens = tokens.T
    half = out_cols // 2
    sent = jnp.concatenate([turned_tokens[:half], turned_tokens[half:]], axis=1)
    got = exchange(jnp.broadcast_to(sent[None], (n_tp, half, LANE)), "tp")

    cos_len, sin_len = angles_of(lengths)
    cos_len = jnp.concatenate([cos_len, cos_len], axis=1)
    sin_len = jnp.concatenate([-sin_len, sin_len], axis=1)
    positions = kv_index * cache_dev + jnp.arange(cache_dev, dtype=jnp.int32)
    cos_pos, sin_pos = angles_of(positions)
    lower = cache_rope[..., : ROPE // 2].astype(F32)
    upper = cache_rope[..., ROPE // 2 :].astype(F32)
    rotated = jnp.concatenate(
        [lower * cos_pos - upper * sin_pos, upper * cos_pos + lower * sin_pos], axis=-1
    ).astype(BF)

    sent, own_tokens = call(
        stage_query,
        [((n_kv, 112, LANE), BF), ((seq_dev, width), F32)],
        [at, got, gain_attn[None], w_query_nope, w_query_rope, w_latent, w_rope_key],
    )
    got = exchange(sent, KV)
    sent, new = call(
        stage_absorb,
        [((n_tp, seq_dev, RANK + LANE), BF), ((seq_dev, RANK + LANE), F32)],
        [at, got, w_key_up, gain_latent[None], cos_len, sin_len],
        [(batch, RANK + LANE), (2, batch, LANE)],
    )
    got = exchange(sent, "tp")
    sent = call(
        stage_attend,
        [((n_tp, seq_dev, RANK + LANE), BF)],
        [at, got, cache_latent, rotated, new],
        [(batch, RANK + LANE)],
    )
    got = exchange(sent, "tp")
    sent = call(
        stage_heads,
        [((n_kv, batch + 16, LANE), BF)],
        [got, w_value_up],
        [(batch, RANK + LANE)],
        scalars=False,
    )
    got = exchange(sent, KV)
    sent = call(
        stage_project,
        [((n_tp, seq_dev, width), BF)],
        [got, w_out],
        [(batch, width)],
        scalars=False,
    )
    got = exchange(sent, "tp")
    sent = call(
        stage_resid, [((n_tp, seq_dev, width), BF)], [got, own_tokens], scalars=False
    )
    got = exchange(sent, "tp")
    sent, own_resid = call(
        stage_up,
        [((n_kv, batch + 8, units), BF), ((out_cols, batch), F32)],
        [at, got, gain_mlp[None], w_up],
        [(batch, width)],
    )
    got = exchange(sent, KV)
    sent = call(stage_down, [((n_tp, half, LANE), BF)], [got, w_down], scalars=False)
    got = exchange(sent, "tp")
    return call(stage_last, [((batch, out_cols), BF)], [got, own_resid], scalars=False)


def solution(mesh):
    split = Mesh(mesh.devices.reshape(4, 4, mesh.shape["tp"]), ("kv_0", "kv_1", "tp"))
    in_specs = (
        P(None, KV_TP),
        P(),
        P(KV),
        P(KV, "tp"),
        P(KV, "tp"),
        P(KV, None),
        P(KV, None),
        P(),
        P(None, "tp"),
        P(None, "tp"),
        P("tp", KV),
        P(KV),
        P(KV, "tp"),
        P("tp", KV),
        P("tp", KV, None),
        P("tp", KV, None),
    )
    out_specs = P(None, KV_TP)
    return jax.shard_map(
        per_device, mesh=split, in_specs=in_specs, out_specs=out_specs, check_vma=False
    )
```

```python
import jax
import jax.numpy as jnp
from jax import lax
from jax.experimental import pallas as pl
from jax.experimental.pallas import tpu as pltpu
from jax.sharding import Mesh
from jax.sharding import PartitionSpec as P

D = 4096
NOPE = 128
ROPE = 64
VD = 128
RANK = 512
LANE = 128
KV = ("kv_0", "kv_1")
KV_TP = ("kv_0", "kv_1", "tp")
EPS = 1e-06
BF = jnp.bfloat16
F32 = jnp.float32
NT = (((1,), (1,)), ((), ()))


def exchange(parts, axis):
    return lax.all_to_all(parts, axis, 0, 0, tiled=True)


def mm(a, b):
    return jnp.dot(a, b, preferred_element_type=F32)


def mm_nt(a, b):
    return lax.dot_general(a, b, NT, preferred_element_type=F32)


def split3(x):
    hi = x.astype(BF).astype(F32)
    rest = x - hi
    mid = rest.astype(BF).astype(F32)
    return hi, mid, rest - mid


def as_column(row):
    n = row.shape[1]
    full = jnp.broadcast_to(row, (LANE, n))
    return jnp.transpose(full)


def kv_at():
    return lax.axis_index("kv_0") * lax.axis_size("kv_1") + lax.axis_index("kv_1")


def tp_at():
    return lax.axis_index("tp")


def one_hot_rows(first, rows, columns):
    row = lax.broadcasted_iota(jnp.int32, (rows, columns), 0)
    column = lax.broadcasted_iota(jnp.int32, (rows, columns), 1)
    return jnp.where(column == first + row, 1.0, 0.0).astype(BF)


def read_pairs(ref, scratch):
    n, two, _ = ref.shape
    for i in range(n):
        scratch[two * i : two * (i + 1), :] = ref[i].astype(F32)
    return scratch[...]


def write_pairs(ref, scratch, value):
    n, two, _ = ref.shape
    scratch[...] = value
    for i in range(n):
        ref[i] = scratch[two * i : two * (i + 1), :].astype(BF)


def stage_send(tokens_t, out):
    x = tokens_t[...].astype(F32)
    half = x.shape[0] // 2
    packed = jnp.concatenate([x[:half], x[half:]], axis=1).astype(BF)
    for j in range(out.shape[0]):
        out[j] = packed


def stage_query(got, gain, w_nope, w_rope_t, w_latent, w_key_t, cos_pos, cos_len, out, own_out):
    del cos_pos, cos_len
    n_tp, four, _ = got.shape
    seq_dev = own_out.shape[0]
    x = got[...].astype(F32)
    batch = LANE // 2
    block_t = jnp.concatenate([x[:, :, :batch], x[:, :, batch:]], axis=1)
    block_t = block_t.reshape(n_tp * 2 * four, batch)
    squares = jnp.sum(block_t * block_t, axis=0, keepdims=True)
    block = jnp.transpose(block_t)
    scaled = (block * gain[...]).astype(BF)
    nope = mm(scaled, w_nope[...])
    rope = mm_nt(scaled, w_rope_t[...])
    pick = one_hot_rows(tp_at() * seq_dev, 8, batch)
    own = mm(pick, scaled).astype(BF)
    own_out[...] = mm(pick, block.astype(BF))[:seq_dev]
    latent = mm(own, w_latent[...])
    key = mm_nt(own, w_key_t[...])
    half = batch // 2
    rows = [
        nope,
        jnp.concatenate([rope[:half], rope[half:]], axis=1),
        *[latent[:2, LANE * j : LANE * (j + 1)] for j in range(RANK // LANE)],
        jnp.concatenate([key[0:1], key[1:2]], axis=1),
        jnp.concatenate([squares, squares], axis=1),
        jnp.zeros((6, LANE), F32),
    ]
    packed = jnp.concatenate(rows, axis=0).astype(BF)
    for j in range(out.shape[0]):
        out[j] = packed


def turned(values, cos_ref, sin_ref):
    half = values.shape[1] // 2
    swapped = jnp.concatenate([values[:, half:], values[:, :half]], axis=1)
    return values * cos_ref + swapped * sin_ref


def stage_absorb(got, w_key_up, gain_latent, cos_ref, sin_ref, out, new_out, scratch, trig):
    cos_len = jnp.concatenate([cos_ref[...], cos_ref[...]], axis=1)
    sin_len = jnp.concatenate([-sin_ref[...], sin_ref[...]], axis=1)
    total = got[0].astype(F32)
    for j in range(1, got.shape[0]):
        total = total + got[j].astype(F32)
    batch = w_key_up.shape[1] // 2
    half = batch // 2
    nope = total[:batch]
    packed = total[batch : batch + half]
    rope = jnp.concatenate([packed[:, :ROPE], packed[:, ROPE:]], axis=0)
    at_row = batch + half
    latent = jnp.concatenate([total[at_row + 2 * j : at_row + 2 * j + 2] for j in range(4)], axis=1)
    key = total[at_row + 8 : at_row + 9]
    key = jnp.concatenate([key[:, :ROPE], key[:, ROPE:]], axis=0)
    squares = total[at_row + 9 : at_row + 10, :batch]
    inv = as_column(lax.rsqrt(squares / D + EPS))
    q_nope = (nope * inv).astype(BF)
    q_rope = turned(rope * inv[:, :ROPE], cos_len, sin_len)
    q_latent = mm_nt(q_nope, w_key_up[...])
    value = jnp.concatenate([q_latent, q_rope, jnp.zeros_like(q_rope)], axis=1)
    write_pairs(out, scratch, value)
    first = tp_at() * 2
    trig[0] = inv
    trig[1] = jnp.concatenate([cos_len, sin_len], axis=1)
    own_inv = trig[0, pl.ds(first, 2), :]
    own_trig = trig[1, pl.ds(first, 2), :]
    raw = latent * own_inv[:, :1]
    norm = lax.rsqrt(jnp.mean(raw * raw, axis=1, keepdims=True) + EPS)
    latent_new = raw * norm * gain_latent[...]
    key_new = turned(key * own_inv[:, :ROPE], own_trig[:, :ROPE], own_trig[:, ROPE:])
    new_out[...] = (
        jnp.concatenate([latent_new, key_new, jnp.zeros_like(key_new)], axis=1)
        .astype(BF)
        .astype(F32)
    )


def stage_attend(lengths, got, cache, rope, cos_pos, sin_pos, new, out, scratch):
    query = read_pairs(got, scratch)
    rows = query.shape[0]
    cache_dev = cache.shape[1]
    latent_query = query[:, :RANK].astype(BF)
    rope_query = query[:, RANK : RANK + ROPE].astype(BF)
    even_column = lax.broadcasted_iota(jnp.int32, (rows, 1), 0) % 2 == 0
    scale = (NOPE + ROPE) ** (-0.5)
    half = ROPE // 2
    each = []
    for s in range(2):
        lower = rope[s, :half].astype(F32)
        upper = rope[s, half:].astype(F32)
        rotated = jnp.concatenate(
            [
                lower * cos_pos[...] - upper * sin_pos[...],
                upper * cos_pos[...] + lower * sin_pos[...],
            ],
            axis=0,
        ).astype(BF)
        each.append(mm_nt(latent_query, cache[s]) + mm(rope_query, rotated))
    scores = jnp.where(even_column, each[0], each[1]) * scale
    length = jnp.where(even_column, lengths[tp_at() * 2], lengths[tp_at() * 2 + 1])
    position = kv_at() * cache_dev + lax.broadcasted_iota(jnp.int32, scores.shape, 1)
    live = position < length
    new_rows = jnp.where(even_column, new[0:1], new[1:2])
    own = jnp.sum(query * new_rows, axis=1, keepdims=True) * scale
    first = kv_at() == 0
    peak = jnp.max(jnp.where(live, scores, -1e30), axis=1, keepdims=True)
    peak = jnp.where(first, jnp.maximum(peak, own), peak)
    expo = jnp.where(live, jnp.exp(scores - peak), 0.0)
    own_weight = jnp.where(first, jnp.exp(own - peak), 0.0)
    mass = jnp.sum(expo, axis=1, keepdims=True) + own_weight
    low = [
        jnp.where(even_column, expo, 0.0).astype(BF),
        jnp.where(even_column, 0.0, expo).astype(BF),
    ]
    weighted = mm(low[0], cache[0]) + mm(low[1], cache[1])
    weighted = weighted + own_weight * new_rows[:, :RANK]
    block_out = weighted / jnp.where(mass > 0, mass, 1.0)
    lane = lax.broadcasted_iota(jnp.int32, (rows, LANE), 1)
    stats = jnp.zeros((rows, LANE), F32)
    for i, piece in enumerate((*split3(peak), *split3(mass))):
        stats = jnp.where(lane == i, piece, stats)
    write_pairs(out, scratch, jnp.concatenate([block_out, stats], axis=1))


def stage_heads(got, w_value_up, out, scratch):
    value = read_pairs(got, scratch)
    part = mm(value[:, :RANK].astype(BF), w_value_up[...])
    stats = jnp.transpose(value[:, RANK:])[:16]
    stats = jnp.concatenate([stats, jnp.zeros_like(stats)], axis=1)
    packed = jnp.concatenate([part, stats], axis=0).astype(BF)
    for j in range(out.shape[0]):
        out[j] = packed


def stage_project(got, w_out, out, scratch):
    blocks, rows, _ = got.shape
    batch = rows - 16
    stats = got[:, batch:, :].astype(F32)
    peak = stats[:, 0] + (stats[:, 1] + stats[:, 2])
    mass = stats[:, 3] + (stats[:, 4] + stats[:, 5])
    top = jnp.max(peak, axis=0, keepdims=True)
    weight = mass * jnp.exp(peak - top)
    total = jnp.sum(weight, axis=0, keepdims=True)
    weight = weight / jnp.where(total > 0, total, 1.0)
    weight = jnp.concatenate([weight, jnp.zeros((LANE - blocks, LANE), F32)], axis=0)
    column = jnp.transpose(weight)[:batch]
    head = column[:, 0:1] * got[0, :batch].astype(F32)
    for j in range(1, blocks):
        head = head + column[:, j : j + 1] * got[j, :batch].astype(F32)
    write_pairs(out, scratch, mm(head.astype(BF), w_out[...]))


def stage_resid(got, own, out):
    total = own[...]
    for i in range(got.shape[0]):
        total = total + got[i].astype(F32)
    total = total.astype(BF)
    for i in range(out.shape[0]):
        out[i] = total


def stage_up(got, gain, w_up, out, own_out, scratch):
    resid = read_pairs(got, scratch)
    batch, width = resid.shape
    squares = jnp.sum(resid * resid, axis=1, keepdims=True)
    square_rows = jnp.transpose(jnp.broadcast_to(squares, (batch, LANE)))[:8]
    scaled = (resid * gain[...]).astype(BF)
    up = mm(scaled, w_up[...])
    units = up.shape[1]
    extra = jnp.concatenate([square_rows, jnp.zeros((8, units - batch), F32)], axis=1)
    packed = jnp.concatenate([up, extra], axis=0).astype(BF)
    for j in range(out.shape[0]):
        out[j] = packed
    pick = one_hot_rows(tp_at() * 8, 8, width)
    own_out[...] = mm_nt(pick, resid.astype(BF))


def stage_down(got, w_down, out):
    total = got[0].astype(F32)
    for j in range(1, got.shape[0]):
        total = total + got[j].astype(F32)
    batch = total.shape[0] - 8
    active = jnp.square(jnp.maximum(total[:batch], 0.0)).astype(BF)
    inv = lax.rsqrt(total[batch : batch + 1, :batch] / D + EPS)
    down = jnp.transpose(mm(active, w_down[...])) * (inv * inv)
    n_tp = out.shape[0]
    down = down.reshape(n_tp, -1, batch)
    half = down.shape[1] // 2
    out[...] = jnp.concatenate([down[:, :half], down[:, half:]], axis=2).astype(BF)


def stage_last(got, own, out):
    total = jnp.sum(got[...].astype(F32), axis=0)
    batch = own.shape[1]
    value = jnp.concatenate([total[:, :batch], total[:, batch:]], axis=0) + own[...]
    out[...] = value.astype(BF)


def call(body, outs, operands, scratch=(), spaces=()):
    specs = [pl.BlockSpec(memory_space=pltpu.VMEM) for _ in operands]
    for index, space in spaces:
        specs[index] = pl.BlockSpec(memory_space=space)
    made = pl.pallas_call(
        body,
        out_shape=[jax.ShapeDtypeStruct(s, t) for s, t in outs],
        in_specs=specs,
        out_specs=[pl.BlockSpec(memory_space=pltpu.VMEM) for _ in outs],
        scratch_shapes=[pltpu.VMEM(s, F32) for s in scratch],
        compiler_params=pltpu.CompilerParams(vmem_limit_bytes=16 * 1024 * 1024),
        name=body.__name__,
    )(*operands)
    return made if len(outs) > 1 else made[0]


def inv_freq():
    half_dim = ROPE // 2
    return 10000.0 ** (-jnp.arange(half_dim, dtype=F32) / half_dim)


def per_device(
    tokens,
    lengths,
    gain_attn,
    w_query_nope,
    w_query_rope,
    w_latent,
    w_rope_key,
    gain_latent,
    w_key_up,
    w_value_up,
    w_out,
    gain_mlp,
    w_up,
    w_down,
    cache_latent,
    cache_rope,
):
    kv_index = lax.axis_index(KV)
    n_kv = lax.axis_size(KV)
    n_tp = lax.axis_size("tp")
    seq_dev, cache_dev = cache_latent.shape[:2]
    batch, out_cols = tokens.shape
    width = w_out.shape[1]
    units = w_up.shape[1]
    half = out_cols // 2

    sent = call(stage_send, [((n_tp, half, LANE), BF)], [tokens.T])
    got = exchange(sent, "tp")

    angles = lengths.astype(F32)[:, None] * inv_freq()
    cos_len, sin_len = jnp.cos(angles), jnp.sin(angles)
    positions = kv_index * cache_dev + jnp.arange(cache_dev, dtype=jnp.int32)
    angles = positions.astype(F32)[None] * inv_freq()[:, None]
    cos_pos, sin_pos = jnp.cos(angles), jnp.sin(angles)
    any_space = pl.ANY

    sent, own_tokens = call(
        stage_query,
        [((n_kv, 112, LANE), BF), ((seq_dev, width), F32)],
        [
            got,
            gain_attn[None],
            w_query_nope,
            w_query_rope.T,
            w_latent,
            w_rope_key.T,
            cos_pos,
            cos_len,
        ],
        spaces=[(6, any_space), (7, any_space)],
    )
    got = exchange(sent, KV)
    sent, new = call(
        stage_absorb,
        [((n_tp, seq_dev, RANK + LANE), BF), ((seq_dev, RANK + LANE), F32)],
        [got, w_key_up, gain_latent[None], cos_len, sin_len],
        [(batch, RANK + LANE), (2, batch, LANE)],
    )
    got = exchange(sent, "tp")
    sent = call(
        stage_attend,
        [((n_tp, seq_dev, RANK + LANE), BF)],
        [lengths, got, cache_latent, jnp.swapaxes(cache_rope, 1, 2), cos_pos, sin_pos, new],
        [(batch, RANK + LANE)],
        [(0, pltpu.SMEM)],
    )
    got = exchange(sent, "tp")
    sent = call(
        stage_heads,
        [((n_kv, batch + 16, LANE), BF)],
        [got, w_value_up],
        [(batch, RANK + LANE)],
    )
    got = exchange(sent, KV)
    sent = call(
        stage_project,
        [((n_tp, seq_dev, width), BF)],
        [got, w_out],
        [(batch, width)],
    )
    got = exchange(sent, "tp")
    sent = call(
        stage_resid, [((n_tp, seq_dev, width), BF)], [got, own_tokens]
    )
    got = exchange(sent, "tp")
    sent, own_resid = call(
        stage_up,
        [((n_kv, batch + 8, units), BF), ((out_cols, batch), F32)],
        [got, gain_mlp[None], w_up],
        [(batch, width)],
    )
    got = exchange(sent, KV)
    sent = call(stage_down, [((n_tp, half, LANE), BF)], [got, w_down])
    got = exchange(sent, "tp")
    return call(stage_last, [((out_cols, batch), BF)], [got, own_resid]).T


def solution(mesh):
    split = Mesh(mesh.devices.reshape(4, 4, mesh.shape["tp"]), ("kv_0", "kv_1", "tp"))
    in_specs = (
        P(None, KV_TP),
        P(),
        P(KV),
        P(KV, "tp"),
        P(KV, "tp"),
        P(KV, None),
        P(KV, None),
        P(),
        P(None, "tp"),
        P(None, "tp"),
        P("tp", KV),
        P(KV),
        P(KV, "tp"),
        P("tp", KV),
        P("tp", KV, None),
        P("tp", KV, None),
    )
    out_specs = P(None, KV_TP)
    return jax.shard_map(
        per_device, mesh=split, in_specs=in_specs, out_specs=out_specs, check_vma=False
    )
```

```python
import jax
import jax.numpy as jnp
from jax import lax
from jax.experimental import pallas as pl
from jax.experimental.pallas import tpu as pltpu
from jax.sharding import Mesh
from jax.sharding import PartitionSpec as P

D = 4096
NOPE = 128
ROPE = 64
VD = 128
RANK = 512
LANE = 128
KV = ("kv_0", "kv_1")
TP = ("far", "near")
KV_TP = ("kv_0", "kv_1", "far", "near")
EPS = 1e-06
BF = jnp.bfloat16
F32 = jnp.float32
NT = (((1,), (1,)), ((), ()))


def exchange(parts, axis):
    return lax.all_to_all(parts, axis, 0, 0, tiled=True)


def mm(a, b):
    return jnp.dot(a, b, preferred_element_type=F32)


def mm_nt(a, b):
    return lax.dot_general(a, b, NT, preferred_element_type=F32)


def split3(x):
    hi = x.astype(BF).astype(F32)
    rest = x - hi
    mid = rest.astype(BF).astype(F32)
    return hi, mid, rest - mid


def as_column(row):
    n = row.shape[1]
    full = jnp.broadcast_to(row, (LANE, n))
    return jnp.transpose(full)


def kv_at():
    return lax.axis_index("kv_0") * lax.axis_size("kv_1") + lax.axis_index("kv_1")


def tp_at():
    return lax.axis_index("far") * lax.axis_size("near") + lax.axis_index("near")


def one_hot_rows(first, rows, columns):
    row = lax.broadcasted_iota(jnp.int32, (rows, columns), 0)
    column = lax.broadcasted_iota(jnp.int32, (rows, columns), 1)
    return jnp.where(column == first + row, 1.0, 0.0).astype(BF)


def read_pairs(ref, scratch):
    n, two, _ = ref.shape
    for i in range(n):
        scratch[two * i : two * (i + 1), :] = ref[i].astype(F32)
    return scratch[...]


def write_pairs(ref, scratch, value):
    n, two, _ = ref.shape
    scratch[...] = value
    for i in range(n):
        ref[i] = scratch[two * i : two * (i + 1), :].astype(BF)


def stage_send(tokens_t, out):
    x = tokens_t[...].astype(F32)
    half = x.shape[0] // 2
    packed = jnp.concatenate([x[:half], x[half:]], axis=1).astype(BF)
    for j in range(out.shape[0]):
        out[j] = packed


def stage_query(got, gain, w_nope, w_rope_t, w_latent, w_key_t, cos_pos, cos_len, out, own_out):
    del cos_pos, cos_len
    n_tp, four, _ = got.shape
    x = got[...].astype(F32)
    batch = LANE // 2
    block_t = jnp.concatenate([x[:, :, :batch], x[:, :, batch:]], axis=1)
    block_t = block_t.reshape(n_tp * 2 * four, batch)
    squares = jnp.sum(block_t * block_t, axis=0, keepdims=True)
    block = jnp.transpose(block_t)
    scaled = (block * gain[...]).astype(BF)
    nope = mm(scaled, w_nope[...])
    rope = mm_nt(scaled, w_rope_t[...])
    own = mm(one_hot_rows(tp_at() * 2, 8, batch), scaled).astype(BF)
    rows = own_out.shape[0]
    own_out[...] = mm(
        one_hot_rows(lax.axis_index("near") * rows, rows, batch), block.astype(BF)
    )
    latent = mm(own, w_latent[...])
    key = mm_nt(own, w_key_t[...])
    half = batch // 2
    rows = [
        nope,
        jnp.concatenate([rope[:half], rope[half:]], axis=1),
        *[latent[:2, LANE * j : LANE * (j + 1)] for j in range(RANK // LANE)],
        jnp.concatenate([key[0:1], key[1:2]], axis=1),
        jnp.concatenate([squares, squares], axis=1),
        jnp.zeros((6, LANE), F32),
    ]
    packed = jnp.concatenate(rows, axis=0).astype(BF)
    for j in range(out.shape[0]):
        out[j] = packed


def turned(values, cos_ref, sin_ref):
    half = values.shape[1] // 2
    swapped = jnp.concatenate([values[:, half:], values[:, :half]], axis=1)
    return values * cos_ref + swapped * sin_ref


def stage_absorb(got, w_key_up, gain_latent, cos_ref, sin_ref, out, new_out, scratch, trig):
    cos_len = jnp.concatenate([cos_ref[...], cos_ref[...]], axis=1)
    sin_len = jnp.concatenate([-sin_ref[...], sin_ref[...]], axis=1)
    total = got[0].astype(F32)
    for j in range(1, got.shape[0]):
        total = total + got[j].astype(F32)
    batch = w_key_up.shape[1] // 2
    half = batch // 2
    nope = total[:batch]
    packed = total[batch : batch + half]
    rope = jnp.concatenate([packed[:, :ROPE], packed[:, ROPE:]], axis=0)
    at_row = batch + half
    latent = jnp.concatenate([total[at_row + 2 * j : at_row + 2 * j + 2] for j in range(4)], axis=1)
    key = total[at_row + 8 : at_row + 9]
    key = jnp.concatenate([key[:, :ROPE], key[:, ROPE:]], axis=0)
    squares = total[at_row + 9 : at_row + 10, :batch]
    inv = as_column(lax.rsqrt(squares / D + EPS))
    q_nope = (nope * inv).astype(BF)
    q_rope = turned(rope * inv[:, :ROPE], cos_len, sin_len)
    q_latent = mm_nt(q_nope, w_key_up[...])
    value = jnp.concatenate([q_latent, q_rope, jnp.zeros_like(q_rope)], axis=1)
    write_pairs(out, scratch, value)
    first = tp_at() * 2
    trig[0] = inv
    trig[1] = jnp.concatenate([cos_len, sin_len], axis=1)
    own_inv = trig[0, pl.ds(first, 2), :]
    own_trig = trig[1, pl.ds(first, 2), :]
    raw = latent * own_inv[:, :1]
    norm = lax.rsqrt(jnp.mean(raw * raw, axis=1, keepdims=True) + EPS)
    latent_new = raw * norm * gain_latent[...]
    key_new = turned(key * own_inv[:, :ROPE], own_trig[:, :ROPE], own_trig[:, ROPE:])
    new_out[...] = (
        jnp.concatenate([latent_new, key_new, jnp.zeros_like(key_new)], axis=1)
        .astype(BF)
        .astype(F32)
    )


def stage_attend(lengths, got, cache, rope, cos_pos, sin_pos, new, out, scratch):
    query = read_pairs(got, scratch)
    rows = query.shape[0]
    cache_dev = cache.shape[1]
    latent_query = query[:, :RANK].astype(BF)
    rope_query = query[:, RANK : RANK + ROPE].astype(BF)
    even_column = lax.broadcasted_iota(jnp.int32, (rows, 1), 0) % 2 == 0
    scale = (NOPE + ROPE) ** (-0.5)
    half = ROPE // 2
    each = []
    for s in range(2):
        lower = rope[s, :half].astype(F32)
        upper = rope[s, half:].astype(F32)
        rotated = jnp.concatenate(
            [
                lower * cos_pos[...] - upper * sin_pos[...],
                upper * cos_pos[...] + lower * sin_pos[...],
            ],
            axis=0,
        ).astype(BF)
        each.append(mm_nt(latent_query, cache[s]) + mm(rope_query, rotated))
    scores = jnp.where(even_column, each[0], each[1]) * scale
    length = jnp.where(even_column, lengths[tp_at() * 2], lengths[tp_at() * 2 + 1])
    position = kv_at() * cache_dev + lax.broadcasted_iota(jnp.int32, scores.shape, 1)
    live = position < length
    new_rows = jnp.where(even_column, new[0:1], new[1:2])
    own = jnp.sum(query * new_rows, axis=1, keepdims=True) * scale
    first = kv_at() == 0
    peak = jnp.max(jnp.where(live, scores, -1e30), axis=1, keepdims=True)
    peak = jnp.where(first, jnp.maximum(peak, own), peak)
    expo = jnp.where(live, jnp.exp(scores - peak), 0.0)
    own_weight = jnp.where(first, jnp.exp(own - peak), 0.0)
    mass = jnp.sum(expo, axis=1, keepdims=True) + own_weight
    low = [
        jnp.where(even_column, expo, 0.0).astype(BF),
        jnp.where(even_column, 0.0, expo).astype(BF),
    ]
    weighted = mm(low[0], cache[0]) + mm(low[1], cache[1])
    weighted = weighted + own_weight * new_rows[:, :RANK]
    block_out = weighted / jnp.where(mass > 0, mass, 1.0)
    lane = lax.broadcasted_iota(jnp.int32, (rows, LANE), 1)
    stats = jnp.zeros((rows, LANE), F32)
    for i, piece in enumerate((*split3(peak), *split3(mass))):
        stats = jnp.where(lane == i, piece, stats)
    write_pairs(out, scratch, jnp.concatenate([block_out, stats], axis=1))


def stage_heads(got, w_value_up, out, scratch):
    value = read_pairs(got, scratch)
    part = mm(value[:, :RANK].astype(BF), w_value_up[...])
    stats = jnp.transpose(value[:, RANK:])[:16]
    stats = jnp.concatenate([stats, jnp.zeros_like(stats)], axis=1)
    packed = jnp.concatenate([part, stats], axis=0).astype(BF)
    for j in range(out.shape[0]):
        out[j] = packed


def stage_project(got, w_out, out):
    blocks, rows, _ = got.shape
    batch = rows - 16
    stats = got[:, batch:, :].astype(F32)
    peak = stats[:, 0] + (stats[:, 1] + stats[:, 2])
    mass = stats[:, 3] + (stats[:, 4] + stats[:, 5])
    top = jnp.max(peak, axis=0, keepdims=True)
    weight = mass * jnp.exp(peak - top)
    total = jnp.sum(weight, axis=0, keepdims=True)
    weight = weight / jnp.where(total > 0, total, 1.0)
    weight = jnp.concatenate([weight, jnp.zeros((LANE - blocks, LANE), F32)], axis=0)
    column = jnp.transpose(weight)[:batch]
    head = column[:, 0:1] * got[0, :batch].astype(F32)
    for j in range(1, blocks):
        head = head + column[:, j : j + 1] * got[j, :batch].astype(F32)
    part = mm(head.astype(BF), w_out[...])
    out[...] = part.reshape(out.shape).astype(BF)


def stage_sum(got, out):
    total = got[0].astype(F32)
    for i in range(1, got.shape[0]):
        total = total + got[i].astype(F32)
    total = total.astype(BF)
    for i in range(out.shape[0]):
        out[i] = total


def stage_resid(got, own, out):
    total = own[...]
    for i in range(got.shape[0]):
        total = total + got[i].astype(F32)
    total = total.astype(BF)
    for i in range(out.shape[0]):
        out[i] = total


def stage_up(got, gain, w_up, out, own_out):
    groups, rows, width = got.shape
    resid = got[...].astype(F32).reshape(groups * rows, width)
    batch, width = resid.shape
    squares = jnp.sum(resid * resid, axis=1, keepdims=True)
    square_rows = jnp.transpose(jnp.broadcast_to(squares, (batch, LANE)))[:8]
    scaled = (resid * gain[...]).astype(BF)
    up = mm(scaled, w_up[...])
    units = up.shape[1]
    extra = jnp.concatenate([square_rows, jnp.zeros((8, units - batch), F32)], axis=1)
    packed = jnp.concatenate([up, extra], axis=0).astype(BF)
    for j in range(out.shape[0]):
        out[j] = packed
    pick = one_hot_rows(tp_at() * 8, 8, width)
    own_out[...] = mm_nt(pick, resid.astype(BF))


def stage_down(got, w_down, out):
    total = got[0].astype(F32)
    for j in range(1, got.shape[0]):
        total = total + got[j].astype(F32)
    batch = total.shape[0] - 8
    active = jnp.square(jnp.maximum(total[:batch], 0.0)).astype(BF)
    inv = lax.rsqrt(total[batch : batch + 1, :batch] / D + EPS)
    down = jnp.transpose(mm(active, w_down[...])) * (inv * inv)
    n_tp = out.shape[0]
    down = down.reshape(n_tp, -1, batch)
    half = down.shape[1] // 2
    out[...] = jnp.concatenate([down[:, :half], down[:, half:]], axis=2).astype(BF)


def stage_last(got, own, out):
    total = jnp.sum(got[...].astype(F32), axis=0)
    batch = own.shape[1]
    value = jnp.concatenate([total[:, :batch], total[:, batch:]], axis=0) + own[...]
    out[...] = value.astype(BF)


COST = pl.CostEstimate(flops=40_000_000_000, transcendentals=0, bytes_accessed=20_000_000)


def call(body, outs, operands, scratch=(), spaces=()):
    specs = [pl.BlockSpec(memory_space=pltpu.VMEM) for _ in operands]
    for index, space in spaces:
        specs[index] = pl.BlockSpec(memory_space=space)
    made = pl.pallas_call(
        body,
        out_shape=[jax.ShapeDtypeStruct(s, t) for s, t in outs],
        in_specs=specs,
        out_specs=[pl.BlockSpec(memory_space=pltpu.VMEM) for _ in outs],
        scratch_shapes=[pltpu.VMEM(s, F32) for s in scratch],
        compiler_params=pltpu.CompilerParams(vmem_limit_bytes=16 * 1024 * 1024),
        cost_estimate=COST,
        name=body.__name__,
    )(*operands)
    return made if len(outs) > 1 else made[0]


def inv_freq():
    half_dim = ROPE // 2
    return 10000.0 ** (-jnp.arange(half_dim, dtype=F32) / half_dim)


def per_device(
    tokens,
    lengths,
    gain_attn,
    w_query_nope,
    w_query_rope,
    w_latent,
    w_rope_key,
    gain_latent,
    w_key_up,
    w_value_up,
    w_out,
    gain_mlp,
    w_up,
    w_down,
    cache_latent,
    cache_rope,
):
    kv_index = lax.axis_index(KV)
    n_kv = lax.axis_size(KV)
    n_tp = lax.axis_size(TP)
    n_near, n_far = lax.axis_size("near"), lax.axis_size("far")
    seq_dev, cache_dev = cache_latent.shape[:2]
    batch, out_cols = tokens.shape
    width = w_out.shape[1]
    units = w_up.shape[1]
    half = out_cols // 2

    sent = call(stage_send, [((n_tp, half, LANE), BF)], [tokens.T])
    got = exchange(sent, TP)

    angles = lengths.astype(F32)[:, None] * inv_freq()
    cos_len, sin_len = jnp.cos(angles), jnp.sin(angles)
    positions = kv_index * cache_dev + jnp.arange(cache_dev, dtype=jnp.int32)
    angles = positions.astype(F32)[None] * inv_freq()[:, None]
    cos_pos, sin_pos = jnp.cos(angles), jnp.sin(angles)
    any_space = pl.ANY

    sent, own_tokens = call(
        stage_query,
        [((n_kv, 112, LANE), BF), ((batch // n_near, width), F32)],
        [
            got,
            gain_attn[None],
            w_query_nope,
            w_query_rope.T,
            w_latent,
            w_rope_key.T,
            cos_pos,
            cos_len,
        ],
        spaces=[(6, any_space), (7, any_space)],
    )
    got = exchange(sent, KV)
    sent, new = call(
        stage_absorb,
        [((n_tp, seq_dev, RANK + LANE), BF), ((seq_dev, RANK + LANE), F32)],
        [got, w_key_up, gain_latent[None], cos_len, sin_len],
        [(batch, RANK + LANE), (2, batch, LANE)],
    )
    got = exchange(sent, TP)
    sent = call(
        stage_attend,
        [((n_tp, seq_dev, RANK + LANE), BF)],
        [lengths, got, cache_latent, jnp.swapaxes(cache_rope, 1, 2), cos_pos, sin_pos, new],
        [(batch, RANK + LANE)],
        [(0, pltpu.SMEM)],
    )
    got = exchange(sent, TP)
    sent = call(
        stage_heads,
        [((n_kv, batch + 16, LANE), BF)],
        [got, w_value_up],
        [(batch, RANK + LANE)],
    )
    got = exchange(sent, KV)
    sent = call(
        stage_project,
        [((n_near, batch // n_near, width), BF)],
        [got, w_out],
    )
    got = exchange(sent, "near")
    sent = call(stage_sum, [((n_far, batch // n_near, width), BF)], [got])
    got = exchange(sent, "far")
    sent = call(stage_resid, [((n_near, batch // n_near, width), BF)], [got, own_tokens])
    got = exchange(sent, "near")
    n_0, n_1 = lax.axis_size("kv_0"), lax.axis_size("kv_1")
    sent, own_resid = call(
        stage_up,
        [((n_1, batch + 8, units), BF), ((out_cols, batch), F32)],
        [got, gain_mlp[None], w_up],
    )
    got = exchange(sent, "kv_1")
    sent = call(stage_sum, [((n_0, batch + 8, units), BF)], [got])
    got = exchange(sent, "kv_0")
    sent = call(stage_down, [((n_tp, half, LANE), BF)], [got, w_down])
    got = exchange(sent, TP)
    return call(stage_last, [((out_cols, batch), BF)], [got, own_resid]).T


def solution(mesh):
    n_tp = mesh.shape["tp"]
    split = Mesh(
        mesh.devices.reshape(4, 4, n_tp // 4, 4), ("kv_0", "kv_1", "far", "near")
    )
    in_specs = (
        P(None, KV_TP),
        P(),
        P(KV),
        P(KV, TP),
        P(KV, TP),
        P(KV, None),
        P(KV, None),
        P(),
        P(None, TP),
        P(None, TP),
        P(TP, KV),
        P(KV),
        P(KV, TP),
        P(TP, KV),
        P(TP, KV, None),
        P(TP, KV, None),
    )
    out_specs = P(None, KV_TP)
    return jax.shard_map(
        per_device, mesh=split, in_specs=in_specs, out_specs=out_specs, check_vma=False
    )
```
